32 devices in a mesh: sp: 16 (over z, y, x), tp: 2 (over core).
Axes of the slice: x: 2, y: 2, z: 4, core: 2. Of those that a mesh axis runs over, the one named last changes fastest.
Arguments:
- skip_pathway: bfloat16 [2048, 2048], P('sp', 'tp'), may hold values from -6 to 6
- request_vectors: bfloat16 [2048, 1024], P('sp', 'tp'), may hold values from -6 to 6
- lookup_address_matrix: bfloat16 [2048, 1024], P('sp', 'tp'), may hold values from -6 to 6
- content_vectors: bfloat16 [2048, 1024], P('sp', 'tp'), may hold values from -6 to 6
- result_valve_matrix: bfloat16 [2048, 1024], P('sp', 'tp'), may hold values from -6 to 6
- shrink_raw_signal: float32 [2, 8, 2048], P(None, 'tp', 'sp'), may hold values from -3.1 to 3.6
- channel_shrink_speed: float32 [2, 8], P(None, 'tp'), may hold values from 2.4414063e-05 to 0.05
- insertion_raw_signal: float32 [2, 8, 2048], P(None, 'tp', 'sp'), may hold values from -8.5 to 2
- extra_shrink_spike: float32 [2, 8, 2048], P(None, 'tp', 'sp'), may hold values from -1.2 to 0
- channel_scaling_vector: float32 [128], replicated, may hold values from 0.1 to 1.9
- final_mapping_matrix: bfloat16 [1024, 2048], P(None, 'tp'), may hold values from -0.1875 to 0.1875
- mixer_scaling_vector: float32 [2048], replicated, may hold values from 0.1 to 1.9
- valve_matrix: bfloat16 [2048, 5120], P('sp', 'tp'), may hold values from -0.125 to 0.125
- widening_matrix: bfloat16 [2048, 5120], P('sp', 'tp'), may hold values from -0.125 to 0.125
- temporal_kernel_entries: float32 [3, 5120], P(None, 'tp'), may hold values from -3 to 3
- narrowing_matrix: bfloat16 [5120, 2048], P('tp', 'sp'), may hold values from -0.078125 to 0.078125
Outputs:
- result: bfloat16 [2048, 2048], P('sp', 'tp')
The draws below stay inside these ranges and needn't reach their ends.
All inputs are finite; a program needn't handle non-finite values.
Results may differ from the reference program's by a relative error of at most 0.009.
Values may be sent and summed in bfloat16 or wider, within the bound.
A program may use at most 128 MiB of HBM per device.

```python
import math
import jax
import jax.numpy as jnp
from jax import lax

D = 2048
H = 8
DK = 128
DV = 128
FF = 5120
BLOCK = 64
TOK_DEV = 128
TOKENS = 2048
N_TP = 2


def head_kinds(key):
    share = 0.5
    return jax.random.bernoulli(jax.random.fold_in(key, 11), share, (2, H))


def draw_channel_shrink_speed(key, part):
    slow_head = head_kinds(key)
    slow_rate = jnp.exp(jax.random.uniform(jax.random.fold_in(key, 12), (2, H), jnp.float32, math.log(0.05), math.log(0.5))) / TOKENS
    fast_rate = jnp.exp(jax.random.uniform(jax.random.fold_in(key, 13), (2, H), jnp.float32, math.log(0.015), math.log(0.05)))
    return jnp.where(slow_head, slow_rate, fast_rate).astype(jnp.float32)


def draw_insertion_raw_signal(key, part):
    slow_head = head_kinds(key)
    base = jax.random.truncated_normal(jax.random.fold_in(key, 14), -2.0, 2.0, (2, H, TOKENS), jnp.float32)
    return jnp.where(slow_head[:, :, None], base - 6.5, base).astype(jnp.float32)


def draw_shrink_raw_signal(key, part):
    base = 0.7 * jax.random.truncated_normal(jax.random.fold_in(key, 15), -3.0, 3.0, (2, H, TOKENS), jnp.float32)
    offsets = jax.random.uniform(jax.random.fold_in(key, 16), (2, 1, TOKENS // TOK_DEV), jnp.float32, -1.0, 1.5)
    return (base + jnp.repeat(offsets, TOK_DEV, axis=2)).astype(jnp.float32)


def draw_extra_shrink_spike(key, part):
    places = jax.random.randint(jax.random.fold_in(key, 17), (2, H, 2), 0, TOKENS)
    amounts = jnp.log(jax.random.uniform(jax.random.fold_in(key, 18), (2, H, 2), jnp.float32, 0.55, 0.8))
    positions = jnp.arange(TOKENS, dtype=jnp.int32)
    hits = positions[None, None, None, :] == places[..., None]
    return jnp.sum(jnp.where(hits, amounts[..., None], 0.0), axis=2).astype(jnp.float32)


def shard_levels(stream_key, extent, pieces, low, high):
    level, own = 1.0, jax.random.fold_in(stream_key, 6)
    for axis_at, blocks in pieces:
        steps = jnp.exp(jax.random.uniform(jax.random.fold_in(own, axis_at), (blocks,), jnp.float32, low / len(pieces), high / len(pieces)))
        level = level * jnp.repeat(steps, extent[axis_at] // blocks).reshape([-1 if axis == axis_at else 1 for axis in range(len(extent))])
    return level


def scatter_about(stream_key, dims, scale, reach, cuts=(), kind=jnp.bfloat16):
    loudness = shard_levels(stream_key, dims, cuts, -0.22, 0.18) if cuts else 1.0
    entries = jax.random.normal(stream_key, dims, jnp.float32) * scale * loudness
    return jnp.minimum(jnp.maximum(entries, -reach), reach).astype(kind)


def setup_inputs(seed: int = 0) -> dict:
    arg_keys = jax.random.split(jax.random.key(seed), 17)
    return {
        "skip_pathway": scatter_about(arg_keys[0], (TOKENS, D), 1.0, 6.0, ((0, 16), (1, 2))),
        "request_vectors": scatter_about(arg_keys[1], (TOKENS, H * DK), 1.0, 6.0, ((0, 16), (1, 2))),
        "lookup_address_matrix": scatter_about(arg_keys[2], (TOKENS, H * DK), 1.0, 6.0, ((0, 16), (1, 2))),
        "content_vectors": scatter_about(arg_keys[3], (TOKENS, H * DV), 1.0, 6.0, ((0, 16), (1, 2))),
        "result_valve_matrix": scatter_about(arg_keys[4], (TOKENS, H * DV), 1.5, 6.0, ((0, 16), (1, 2))),
        "shrink_raw_signal": draw_shrink_raw_signal(jax.random.fold_in(arg_keys[16], 71), 0),
        "channel_shrink_speed": draw_channel_shrink_speed(jax.random.fold_in(arg_keys[16], 71), 0),
        "insertion_raw_signal": draw_insertion_raw_signal(jax.random.fold_in(arg_keys[16], 71), 0),
        "extra_shrink_spike": draw_extra_shrink_spike(jax.random.fold_in(arg_keys[16], 71), 0),
        "channel_scaling_vector": jnp.clip(1.0 + 0.18 * jax.random.normal(arg_keys[9], (DV,), jnp.float32), 0.1, 1.9),
        "final_mapping_matrix": scatter_about(arg_keys[10], (H * DV, D), (H * DV) ** -0.5, 0.1875, ((1, 2),)),
        "mixer_scaling_vector": jnp.clip(1.0 + 0.18 * jax.random.normal(arg_keys[11], (D,), jnp.float32), 0.1, 1.9),
        "valve_matrix": scatter_about(arg_keys[12], (D, FF), D ** -0.5, 0.125, ((0, 16), (1, 2))),
        "widening_matrix": scatter_about(arg_keys[13], (D, FF), D ** -0.5, 0.125, ((0, 16), (1, 2))),
        "temporal_kernel_entries": scatter_about(arg_keys[14], (3, FF), 0.5, 3.0, ((1, 2),), jnp.float32),
        "narrowing_matrix": scatter_about(arg_keys[15], (FF, D), FF ** -0.5, 0.078125, ((0, 2), (1, 16))),
    }


HIGHEST = lax.Precision.HIGHEST

def heads_of(matrix, head_size):
    return jnp.transpose(matrix.astype(jnp.float32).reshape(matrix.shape[0], -1, head_size), (1, 0, 2))

def unit_rows(vectors):
    return vectors * lax.rsqrt(lax.optimization_barrier(jnp.sum(vectors * vectors, axis=-1, keepdims=True)) + 1e-06)

def inverse_unit_lower(strict):
    width = strict.shape[-1]
    identity = jnp.eye(width, dtype=jnp.float32)
    powered = -strict
    result = identity + powered
    covered = 2
    while covered < width:
        powered = jnp.matmul(powered, powered, precision=HIGHEST)
        result = jnp.matmul(result, identity + powered, precision=HIGHEST)
        covered = covered * 2
    return result

def block_parts(queries, keys, values, shrink_exponent, beta, width):
    heads, length, key_size = queries.shape
    value_size = values.shape[-1]
    count = length // width
    queries = queries.reshape(heads, count, width, key_size)
    keys = keys.reshape(heads, count, width, key_size)
    values = values.reshape(heads, count, width, value_size)
    shrink_exponent = shrink_exponent.reshape(heads, count, width)
    beta = beta.reshape(heads, count, width)
    cumulative = jnp.cumsum(shrink_exponent, axis=-1)
    inside = jnp.tril(jnp.ones((width, width), dtype=bool))
    decay = jnp.exp(jnp.where(inside, cumulative[..., :, None] - cumulative[..., None, :], -jnp.inf))
    weighted = keys * beta[..., None]
    strict = jnp.tril(jnp.einsum('hnid,hnjd->hnij', weighted, keys, precision=HIGHEST) * decay, -1)
    inverse = inverse_unit_lower(strict)
    writes = jnp.matmul(inverse, values * beta[..., None], precision=HIGHEST)
    erases = jnp.matmul(inverse, weighted * jnp.exp(cumulative)[..., None], precision=HIGHEST)
    within = jnp.einsum('hnid,hnjd->hnij', queries, keys, precision=HIGHEST) * decay
    query_decayed = queries * jnp.exp(cumulative)[..., None]
    keys_decayed = keys * jnp.exp(cumulative[..., -1:] - cumulative)[..., None]
    block_decay = jnp.exp(cumulative[..., -1])
    return (query_decayed, keys_decayed, erases, writes, within, block_decay)

def run_blocks(parts, state):

    def advance(carry, block):
        query_decayed, keys_decayed, erases, writes, within, block_decay = block
        fresh = writes - jnp.matmul(erases, carry, precision=HIGHEST)
        output = jnp.matmul(query_decayed, carry, precision=HIGHEST) + jnp.matmul(within, fresh, precision=HIGHEST)
        carry = carry * block_decay[:, None, None] + jnp.matmul(jnp.swapaxes(keys_decayed, -1, -2), fresh, precision=HIGHEST)
        return (carry, output)
    blocks = tuple((jnp.moveaxis(item, 1, 0) for item in parts))
    final, outputs = lax.scan(advance, state, blocks)
    outputs = jnp.moveaxis(outputs, 0, 1)
    return outputs.reshape(outputs.shape[0], -1, outputs.shape[-1])

def gate_heads(mixture, result_valve_matrix, channel_scaling_vector):
    scaled = mixture * lax.rsqrt(lax.optimization_barrier(jnp.mean(mixture * mixture, axis=-1, keepdims=True)) + 1e-06) * channel_scaling_vector
    gated = scaled * jax.nn.silu(heads_of(result_valve_matrix, mixture.shape[-1]))
    return jnp.transpose(gated, (1, 0, 2)).reshape(gated.shape[1], -1).astype(jnp.bfloat16)

def rms_rows(rows, gain):
    widened = rows.astype(jnp.float32)
    return (widened * lax.rsqrt(lax.optimization_barrier(jnp.mean(widened * widened, axis=-1, keepdims=True)) + 1e-06) * gain).astype(jnp.bfloat16)

def reference(skip_pathway, request_vectors, lookup_address_matrix, content_vectors, result_valve_matrix, shrink_raw_signal, channel_shrink_speed, insertion_raw_signal, extra_shrink_spike, channel_scaling_vector, final_mapping_matrix, mixer_scaling_vector, valve_matrix, widening_matrix, temporal_kernel_entries, narrowing_matrix):
    queries = unit_rows(heads_of(request_vectors, DK)) * DK ** (-0.5)
    keys = unit_rows(heads_of(lookup_address_matrix, DK))
    values = heads_of(content_vectors, DV)
    shrink_exponent = -channel_shrink_speed[:, :, None] * jax.nn.softplus(shrink_raw_signal) + extra_shrink_spike
    beta = jax.nn.sigmoid(insertion_raw_signal)
    empty = jnp.zeros((H, DK, DV), jnp.float32)
    forward = run_blocks(block_parts(queries, keys, values, shrink_exponent[0], beta[0], BLOCK), empty)
    flipped = block_parts(jnp.flip(queries, 1), jnp.flip(keys, 1), jnp.flip(values, 1), jnp.flip(shrink_exponent[1], 1), jnp.flip(beta[1], 1), BLOCK)
    backward = jnp.flip(run_blocks(flipped, empty), 1)
    mixed = gate_heads(forward + backward, result_valve_matrix, channel_scaling_vector)
    projected = jnp.dot(mixed, final_mapping_matrix, preferred_element_type=jnp.float32)
    middle = (skip_pathway.astype(jnp.float32) + projected).astype(jnp.bfloat16)
    normed = rms_rows(middle, mixer_scaling_vector)
    gate = jnp.dot(normed, valve_matrix, preferred_element_type=jnp.float32).astype(jnp.bfloat16)
    up = jnp.dot(normed, widening_matrix, preferred_element_type=jnp.float32)
    padded = jnp.pad(gate, ((1, 1), (0, 0))).astype(jnp.float32)
    convolved = padded[:-2] * temporal_kernel_entries[0] + padded[1:-1] * temporal_kernel_entries[1] + padded[2:] * temporal_kernel_entries[2]
    hidden = (jax.nn.silu(convolved) * up).astype(jnp.bfloat16)
    group = FF // N_TP
    down = jnp.zeros((TOKENS, D), jnp.float32)
    for index in range(N_TP):
        partial_value = jnp.dot(hidden[:, index * group:(index + 1) * group], narrowing_matrix[index * group:(index + 1) * group], preferred_element_type=jnp.float32).astype(jnp.bfloat16)
        partial_value = lax.optimization_barrier(partial_value)
        down = down + partial_value.astype(jnp.float32)
    return (middle.astype(jnp.float32) + down).astype(jnp.bfloat16)
```

```python
import functools

import jax
import jax.numpy as jnp
from jax import lax
from jax.experimental import pallas as pl
from jax.experimental.pallas import tpu as pltpu
from jax.sharding import PartitionSpec as P

DK = 128
DV = 128

HIGH = lax.Precision.HIGH


def heads_of(matrix, head_size):
    return jnp.transpose(
        matrix.astype(jnp.float32).reshape(matrix.shape[0], -1, head_size), (1, 0, 2)
    )


def unit_rows(vectors):
    return vectors * lax.rsqrt(jnp.sum(vectors * vectors, axis=-1, keepdims=True) + 1e-06)


def inverse_unit_triangular(strict):
    width = strict.shape[-1]
    identity = jnp.eye(width, dtype=jnp.float32)
    powered = -strict
    result = identity + powered
    covered = 2
    while covered < width:
        powered = jnp.matmul(powered, powered, precision=HIGH)
        result = result + jnp.matmul(result, powered, precision=HIGH)
        covered = covered * 2
    return result


def local_parts(queries, keys, values, shrink_exponent, beta):
    length = queries.shape[1]
    row = lax.broadcasted_iota(jnp.int32, (length, length), 0)
    column = lax.broadcasted_iota(jnp.int32, (length, length), 1)
    inside = jnp.stack([column <= row, column >= row])[:, None]
    proper = jnp.stack([column < row, column > row])[:, None]
    cumulative = jnp.sum(jnp.where(inside, shrink_exponent[:, :, None, :], 0.0), axis=-1)
    total = jnp.sum(shrink_exponent, axis=-1, keepdims=True)
    decay = jnp.exp(
        jnp.where(inside, cumulative[..., :, None] - cumulative[..., None, :], -jnp.inf)
    )
    likeness = jnp.einsum("hid,hjd->hij", keys, keys, precision=HIGH)
    asked = jnp.einsum("hid,hjd->hij", queries, keys, precision=HIGH)
    strict = jnp.where(proper, likeness * decay * beta[..., None], 0.0)
    inverse = inverse_unit_triangular(strict)
    lift = jnp.exp(cumulative)[..., None]
    right = jnp.concatenate(
        [values * beta[..., None], keys * (beta[..., None] * lift)], axis=-1
    )
    solved = jnp.matmul(inverse, right, precision=HIGH)
    within = asked * decay
    keys_decayed = keys * jnp.exp(total - cumulative)[..., None]
    seen = jnp.matmul(within, solved, precision=HIGH)
    kept = jnp.einsum("ghti,ghtj->ghji", keys_decayed, solved, precision=HIGH)
    dv = values.shape[-1]
    start = jnp.sum(seen[..., :dv], axis=0)
    reach = queries * lift - seen[..., dv:]
    return start, reach, kept, total


def relay_kernel(n, per_direction, dk, maps_ref, out_ref):
    backward = lax.axis_index("sp") >= per_direction
    state = jnp.zeros(out_ref.shape[1:], jnp.float32)
    for step in range(n):
        at = jnp.where(backward, n - 1 - step, step)
        out_ref[at] = state.astype(out_ref.dtype)
        if step < n - 1:
            change = maps_ref[at, :dk, :]
            added = maps_ref[at, dk:, :].astype(jnp.float32)
            upper = state.astype(jnp.bfloat16)
            lower = (state - upper.astype(jnp.float32)).astype(jnp.bfloat16)
            moved = jnp.dot(upper, change, preferred_element_type=jnp.float32)
            moved = moved + jnp.dot(lower, change, preferred_element_type=jnp.float32)
            state = state + moved + added


def entering_states(change, added):
    n = lax.axis_size("sp")
    heads, dk = change.shape[1], change.shape[-1]
    dv = added.shape[2]
    share = n // (2 * heads)
    piece = dv // share
    maps = jnp.concatenate(
        [
            jnp.broadcast_to(change[:, :, None], (2, heads, share, dk, dk)),
            added.reshape(2, heads, share, piece, dk),
        ],
        axis=3,
    ).astype(jnp.bfloat16)
    maps = lax.all_to_all(maps.reshape(n, dk + piece, dk), "sp", 0, 0, tiled=True)
    states = pl.pallas_call(
        functools.partial(relay_kernel, n, n // 2, dk),
        out_shape=jax.ShapeDtypeStruct((n, piece, dk), jnp.bfloat16),
        in_specs=[pl.BlockSpec(memory_space=pltpu.VMEM)],
        out_specs=pl.BlockSpec(memory_space=pltpu.VMEM),
    )(maps)
    states = lax.all_to_all(states, "sp", 0, 0, tiled=True)
    return states.reshape(2, heads, dv, dk)


def gate_heads(mixture, result_valve_matrix, channel_scaling_vector):
    scaled = (
        mixture
        * lax.rsqrt(jnp.mean(mixture * mixture, axis=-1, keepdims=True) + 1e-06)
        * channel_scaling_vector
    )
    gated = scaled * jax.nn.silu(heads_of(result_valve_matrix, mixture.shape[-1]))
    return jnp.transpose(gated, (1, 0, 2)).reshape(gated.shape[1], -1).astype(jnp.bfloat16)


def rms_rows(rows, gain):
    widened = rows.astype(jnp.float32)
    return (
        widened * lax.rsqrt(jnp.mean(widened * widened, axis=-1, keepdims=True) + 1e-06) * gain
    ).astype(jnp.bfloat16)


def group_size(n):
    size = 1
    while 4 * size * size <= n:
        size = size * 2
    return size


def trade(pieces_for, stride, count):
    n = lax.axis_size("sp")
    place = lax.rem(lax.axis_index("sp") // stride, count)
    own = pieces_for(place)
    gathered = lax.dynamic_update_index_in_dim(
        jnp.zeros((count,) + own.shape, own.dtype), own, place, 0
    )
    for flip in range(1, count):
        other = lax.bitwise_xor(place, flip)
        route = [(s, s + ((((s // stride) % count) ^ flip) - (s // stride) % count) * stride) for s in range(n)]
        arrived = lax.ppermute(pieces_for(other), "sp", route)
        gathered = lax.dynamic_update_index_in_dim(gathered, arrived, other, 0)
    return gathered


def swap_within(array, dim, group):
    width = array.shape[dim] // group
    return trade(
        lambda member: lax.dynamic_slice_in_dim(array, member * width, width, axis=dim),
        1,
        group,
    )


def body(
    skip_pathway,
    request_vectors,
    lookup_address_matrix,
    content_vectors,
    result_valve_matrix,
    shrink_raw_signal,
    channel_shrink_speed,
    insertion_raw_signal,
    extra_shrink_spike,
    channel_scaling_vector,
    final_mapping_matrix,
    mixer_scaling_vector,
    valve_matrix,
    widening_matrix,
    temporal_kernel_entries,
    narrowing_matrix,
):
    n = lax.axis_size("sp")
    group = group_size(n)
    place = lax.rem(lax.axis_index("sp"), group)
    far = [[o * group + i for o in range(n // group)] for i in range(group)]

    def collect(pieces):
        return lax.all_gather(pieces, "sp", axis=0, tiled=True, axis_index_groups=far)

    valve = swap_within(valve_matrix, 1, group)
    widening = swap_within(widening_matrix, 1, group)
    valve, widening, request_vectors, lookup_address_matrix = lax.optimization_barrier(
        (valve, widening, request_vectors, lookup_address_matrix)
    )
    valve = collect(valve)
    valve = valve.reshape(-1, valve.shape[-1])
    widening = collect(widening)
    widening = widening.reshape(-1, widening.shape[-1])
    narrowing = swap_within(narrowing_matrix, 0, group)
    units = valve.shape[-1]
    taps = lax.dynamic_slice_in_dim(temporal_kernel_entries, place * units, units, axis=1)

    queries = unit_rows(heads_of(request_vectors, DK)) * DK ** (-0.5)
    keys = unit_rows(heads_of(lookup_address_matrix, DK))
    values = heads_of(content_vectors, DV)
    shrink_exponent = (
        -channel_shrink_speed[:, :, None] * jax.nn.softplus(shrink_raw_signal) + extra_shrink_spike
    )
    beta = jax.nn.sigmoid(insertion_raw_signal)
    start, reach, kept, total = local_parts(queries, keys, values, shrink_exponent, beta)
    added = kept[:, :, :DV]
    change = (
        jnp.expm1(total)[..., None] * jnp.eye(DK, dtype=jnp.float32) - kept[:, :, DV:]
    )
    states = entering_states(change, added)
    narrowing_part, states = lax.optimization_barrier((narrowing, states))
    narrowing = trade(lambda member: narrowing_part, group, n // group)
    narrowing = narrowing.reshape((n,) + narrowing.shape[2:])
    carried = jnp.einsum(
        "ghtk,ghvk->ghtv",
        reach.astype(jnp.bfloat16),
        states,
        preferred_element_type=jnp.float32,
    )
    mixture = start + carried[0] + carried[1]
    mixed = gate_heads(mixture, result_valve_matrix, channel_scaling_vector)
    projected = jnp.dot(
        lax.all_gather(mixed, "tp", axis=1, tiled=True),
        final_mapping_matrix,
        preferred_element_type=jnp.float32,
    )
    middle = (skip_pathway.astype(jnp.float32) + projected).astype(jnp.bfloat16)
    rows = trade(lambda member: middle, 1, group)
    full_rows = jnp.concatenate(
        [lax.all_gather(rows[i], "tp", axis=1, tiled=True) for i in range(group)], axis=0
    )
    normed = rms_rows(full_rows, mixer_scaling_vector)

    gate = jnp.dot(normed, valve, preferred_element_type=jnp.float32).astype(jnp.bfloat16)
    before = lax.ppermute(gate[-1:], "sp", [(s, s + group) for s in range(n - group)])
    after = lax.ppermute(gate[:1], "sp", [(s + group, s) for s in range(n - group)])
    up = jnp.dot(normed, widening, preferred_element_type=jnp.float32)
    padded = jnp.concatenate([before, gate, after], axis=0).astype(jnp.float32)
    convolved = padded[:-2] * taps[0] + padded[1:-1] * taps[1] + padded[2:] * taps[2]
    hidden = (jax.nn.silu(convolved) * up).astype(jnp.bfloat16)
    terms = jnp.einsum(
        "th,nhf->tnf", hidden, narrowing, preferred_element_type=jnp.float32
    ).reshape(hidden.shape[0], -1)
    summed = lax.psum_scatter(
        terms.astype(jnp.bfloat16), "tp", scatter_dimension=1, tiled=True
    )
    summed_parts = summed.reshape((group, -1) + summed.shape[1:])
    summed = trade(
        lambda member: lax.dynamic_index_in_dim(summed_parts, member, 0, keepdims=False),
        1,
        group,
    )
    summed = jnp.sum(summed.astype(jnp.float32), axis=0)
    return (middle.astype(jnp.float32) + summed).astype(jnp.bfloat16)


def solution(mesh):
    return jax.shard_map(
        body,
        mesh=mesh,
        in_specs=(
            P("sp", "tp"),
            P("sp", "tp"),
            P("sp", "tp"),
            P("sp", "tp"),
            P("sp", "tp"),
            P(None, "tp", "sp"),
            P(None, "tp"),
            P(None, "tp", "sp"),
            P(None, "tp", "sp"),
            P(),
            P(None, "tp"),
            P(),
            P("sp", "tp"),
            P("sp", "tp"),
            P(None, "tp"),
            P("tp", "sp"),
        ),
        out_specs=P("sp", "tp"),
        check_vma=False,
    )
```

```python
import functools

import jax
import jax.numpy as jnp
from jax import lax
from jax.experimental import pallas as pl
from jax.experimental.pallas import tpu as pltpu
from jax.sharding import PartitionSpec as P

DK = 128
DV = 128

HIGH = lax.Precision.HIGH


def heads_of(matrix, head_size):
    return jnp.transpose(
        matrix.astype(jnp.float32).reshape(matrix.shape[0], -1, head_size), (1, 0, 2)
    )


def unit_rows(vectors):
    return vectors * lax.rsqrt(jnp.sum(vectors * vectors, axis=-1, keepdims=True) + 1e-06)


def inverse_unit_triangular(strict):
    width = strict.shape[-1]
    identity = jnp.eye(width, dtype=jnp.float32)
    powered = -strict
    result = identity + powered
    covered = 2
    while covered < width:
        powered = jnp.matmul(powered, powered, precision=HIGH)
        result = result + jnp.matmul(result, powered, precision=HIGH)
        covered = covered * 2
    return result


def local_parts(queries, keys, values, shrink_exponent, beta):
    length = queries.shape[1]
    row = lax.broadcasted_iota(jnp.int32, (length, length), 0)
    column = lax.broadcasted_iota(jnp.int32, (length, length), 1)
    inside = jnp.stack([column <= row, column >= row])[:, None]
    proper = jnp.stack([column < row, column > row])[:, None]
    cumulative = jnp.sum(jnp.where(inside, shrink_exponent[:, :, None, :], 0.0), axis=-1)
    total = jnp.sum(shrink_exponent, axis=-1, keepdims=True)
    decay = jnp.exp(
        jnp.where(inside, cumulative[..., :, None] - cumulative[..., None, :], -jnp.inf)
    )
    likeness = jnp.einsum("hid,hjd->hij", keys, keys, precision=HIGH)
    asked = jnp.einsum("hid,hjd->hij", queries, keys, precision=HIGH)
    strict = jnp.where(proper, likeness * decay * beta[..., None], 0.0)
    inverse = inverse_unit_triangular(strict)
    lift = jnp.exp(cumulative)[..., None]
    right = jnp.concatenate(
        [values * beta[..., None], keys * (beta[..., None] * lift)], axis=-1
    )
    solved = jnp.matmul(inverse, right, precision=HIGH)
    within = asked * decay
    keys_decayed = keys * jnp.exp(total - cumulative)[..., None]
    seen = jnp.matmul(within, solved, precision=HIGH)
    kept = jnp.einsum("ghti,ghtj->ghji", keys_decayed, solved, precision=HIGH)
    dv = values.shape[-1]
    start = jnp.sum(seen[..., :dv], axis=0)
    reach = queries * lift - seen[..., dv:]
    return start, reach, kept, total


def relay_kernel(n, per_direction, dk, maps_ref, out_ref):
    backward = lax.axis_index("sp") >= per_direction
    state = jnp.zeros(out_ref.shape[1:], jnp.float32)
    for step in range(n):
        at = jnp.where(backward, n - 1 - step, step)
        out_ref[at] = state.astype(out_ref.dtype)
        if step < n - 1:
            change = maps_ref[at, :dk, :]
            added = maps_ref[at, dk:, :].astype(jnp.float32)
            upper = state.astype(jnp.bfloat16)
            lower = (state - upper.astype(jnp.float32)).astype(jnp.bfloat16)
            moved = jnp.dot(upper, change, preferred_element_type=jnp.float32)
            moved = moved + jnp.dot(lower, change, preferred_element_type=jnp.float32)
            state = state + moved + added


def entering_states(change, added):
    n = lax.axis_size("sp")
    heads, dk = change.shape[1], change.shape[-1]
    dv = added.shape[2]
    share = n // (2 * heads)
    piece = dv // share
    maps = jnp.concatenate(
        [
            jnp.broadcast_to(change[:, :, None], (2, heads, share, dk, dk)),
            added.reshape(2, heads, share, piece, dk),
        ],
        axis=3,
    ).astype(jnp.bfloat16)
    maps = lax.all_to_all(maps.reshape(n, dk + piece, dk), "sp", 0, 0, tiled=True)
    states = pl.pallas_call(
        functools.partial(relay_kernel, n, n // 2, dk),
        out_shape=jax.ShapeDtypeStruct((n, piece, dk), jnp.bfloat16),
        in_specs=[pl.BlockSpec(memory_space=pltpu.VMEM)],
        out_specs=pl.BlockSpec(memory_space=pltpu.VMEM),
    )(maps)
    states = lax.all_to_all(states, "sp", 0, 0, tiled=True)
    return states.reshape(2, heads, dv, dk)


def gate_heads(mixture, result_valve_matrix, channel_scaling_vector):
    scaled = (
        mixture
        * lax.rsqrt(jnp.mean(mixture * mixture, axis=-1, keepdims=True) + 1e-06)
        * channel_scaling_vector
    )
    gated = scaled * jax.nn.silu(heads_of(result_valve_matrix, mixture.shape[-1]))
    return jnp.transpose(gated, (1, 0, 2)).reshape(gated.shape[1], -1).astype(jnp.bfloat16)


def rms_rows(rows, gain):
    widened = rows.astype(jnp.float32)
    return (
        widened * lax.rsqrt(jnp.mean(widened * widened, axis=-1, keepdims=True) + 1e-06) * gain
    ).astype(jnp.bfloat16)


def group_size(n):
    size = 1
    while 4 * size * size <= n:
        size = size * 2
    return size


def trade(pieces_for, stride, count):
    n = lax.axis_size("sp")
    place = lax.rem(lax.axis_index("sp") // stride, count)
    own = pieces_for(place)
    gathered = lax.dynamic_update_index_in_dim(
        jnp.zeros((count,) + own.shape, own.dtype), own, place, 0
    )
    for flip in range(1, count):
        other = lax.bitwise_xor(place, flip)
        route = [(s, s + ((((s // stride) % count) ^ flip) - (s // stride) % count) * stride) for s in range(n)]
        arrived = lax.ppermute(pieces_for(other), "sp", route)
        gathered = lax.dynamic_update_index_in_dim(gathered, arrived, other, 0)
    return gathered


def swap_within(array, dim, group):
    width = array.shape[dim] // group
    return trade(
        lambda member: lax.dynamic_slice_in_dim(array, member * width, width, axis=dim),
        1,
        group,
    )


def body(
    skip_pathway,
    request_vectors,
    lookup_address_matrix,
    content_vectors,
    result_valve_matrix,
    shrink_raw_signal,
    channel_shrink_speed,
    insertion_raw_signal,
    extra_shrink_spike,
    channel_scaling_vector,
    final_mapping_matrix,
    mixer_scaling_vector,
    valve_matrix,
    widening_matrix,
    temporal_kernel_entries,
    narrowing_matrix,
):
    n = lax.axis_size("sp")
    group = group_size(n)
    place = lax.rem(lax.axis_index("sp"), group)
    far = [[o * group + i for o in range(n // group)] for i in range(group)]

    def collect(pieces):
        return lax.all_gather(pieces, "sp", axis=0, tiled=True, axis_index_groups=far)

    valve = swap_within(valve_matrix, 1, group)
    widening = swap_within(widening_matrix, 1, group)
    valve, widening, request_vectors, lookup_address_matrix = lax.optimization_barrier(
        (valve, widening, request_vectors, lookup_address_matrix)
    )
    valve = collect(valve)
    valve = valve.reshape(-1, valve.shape[-1])
    widening = collect(widening)
    widening = widening.reshape(-1, widening.shape[-1])
    narrowing = collect(swap_within(narrowing_matrix, 0, group))
    units = valve.shape[-1]
    taps = lax.dynamic_slice_in_dim(temporal_kernel_entries, place * units, units, axis=1)

    queries = unit_rows(heads_of(request_vectors, DK)) * DK ** (-0.5)
    keys = unit_rows(heads_of(lookup_address_matrix, DK))
    values = heads_of(content_vectors, DV)
    shrink_exponent = (
        -channel_shrink_speed[:, :, None] * jax.nn.softplus(shrink_raw_signal) + extra_shrink_spike
    )
    beta = jax.nn.sigmoid(insertion_raw_signal)
    start, reach, kept, total = local_parts(queries, keys, values, shrink_exponent, beta)
    added = kept[:, :, :DV]
    change = (
        jnp.expm1(total)[..., None] * jnp.eye(DK, dtype=jnp.float32) - kept[:, :, DV:]
    )
    states = entering_states(change, added)
    carried = jnp.einsum(
        "ghtk,ghvk->ghtv",
        reach.astype(jnp.bfloat16),
        states,
        preferred_element_type=jnp.float32,
    )
    mixture = start + carried[0] + carried[1]
    mixed = gate_heads(mixture, result_valve_matrix, channel_scaling_vector)
    projected = jnp.dot(
        lax.all_gather(mixed, "tp", axis=1, tiled=True),
        final_mapping_matrix,
        preferred_element_type=jnp.float32,
    )
    middle = (skip_pathway.astype(jnp.float32) + projected).astype(jnp.bfloat16)
    rows = trade(lambda member: middle, 1, group)
    full_rows = jnp.concatenate(
        [lax.all_gather(rows[i], "tp", axis=1, tiled=True) for i in range(group)], axis=0
    )
    normed = rms_rows(full_rows, mixer_scaling_vector)

    gate = jnp.dot(normed, valve, preferred_element_type=jnp.float32).astype(jnp.bfloat16)
    before = lax.ppermute(gate[-1:], "sp", [(s, s + group) for s in range(n - group)])
    after = lax.ppermute(gate[:1], "sp", [(s + group, s) for s in range(n - group)])
    up = jnp.dot(normed, widening, preferred_element_type=jnp.float32)
    padded = jnp.concatenate([before, gate, after], axis=0).astype(jnp.float32)
    convolved = padded[:-2] * taps[0] + padded[1:-1] * taps[1] + padded[2:] * taps[2]
    hidden = (jax.nn.silu(convolved) * up).astype(jnp.bfloat16)
    terms = jnp.einsum(
        "th,nhf->tnf", hidden, narrowing, preferred_element_type=jnp.float32
    ).reshape(hidden.shape[0], -1)
    summed = lax.psum_scatter(
        terms.astype(jnp.bfloat16), "tp", scatter_dimension=1, tiled=True
    )
    summed_parts = summed.reshape((group, -1) + summed.shape[1:])
    summed = trade(
        lambda member: lax.dynamic_index_in_dim(summed_parts, member, 0, keepdims=False),
        1,
        group,
    )
    summed = jnp.sum(summed.astype(jnp.float32), axis=0)
    return (middle.astype(jnp.float32) + summed).astype(jnp.bfloat16)


def solution(mesh):
    return jax.shard_map(
        body,
        mesh=mesh,
        in_specs=(
            P("sp", "tp"),
            P("sp", "tp"),
            P("sp", "tp"),
            P("sp", "tp"),
            P("sp", "tp"),
            P(None, "tp", "sp"),
            P(None, "tp"),
            P(None, "tp", "sp"),
            P(None, "tp", "sp"),
            P(),
            P(None, "tp"),
            P(),
            P("sp", "tp"),
            P("sp", "tp"),
            P(None, "tp"),
            P("tp", "sp"),
        ),
        out_specs=P("sp", "tp"),
        check_vma=False,
    )
```
